32 devices in a mesh: fs: 4 (over y, x), tp: 8 (over z, core).
Axes of the slice: x: 2, y: 2, z: 4, core: 2. Of those that a mesh axis runs over, the one named last changes fastest.
Arguments:
- tokens: bfloat16 [4096, 2048], P(('fs', 'tp')), may hold values from -6 to 6
- gain: float32 [2048], P('fs'), may hold values from 0.1 to 1.9
- ex_gate: float32 [8, 256, 2048], P('tp', None, 'fs'), may hold values from -0.125 to 0.125
- ex_up: float32 [8, 256, 2048], P('tp', None, 'fs'), may hold values from -0.125 to 0.125
- ex_down: float32 [8, 256, 2048], P('tp', None, 'fs'), may hold values from -0.375 to 0.375
- sh_gate: float32 [512, 2048], P('tp', 'fs'), may hold values from -0.125 to 0.125
- sh_up: float32 [512, 2048], P('tp', 'fs'), may hold values from -0.125 to 0.125
- sh_down: float32 [512, 2048], P('tp', 'fs'), may hold values from -0.25 to 0.25
- routes: int32 [4096, 4], P(('fs', 'tp')), may hold values from 0 to 7, all different within a row; in each aligned block of 128 rows (0 to 127, 128 to 255, ...) at most 72 rows name the same one
- route_weight: float32 [4096, 4], P(('fs', 'tp')), may hold values from 0.1 to 1
Outputs:
- mixed: bfloat16 [4096, 2048], P(('fs', 'tp'))
- expert_gate: bfloat16 [8, 256, 2048], P('tp')
- expert_up: bfloat16 [8, 256, 2048], P('tp')
- expert_down: bfloat16 [8, 256, 2048], P('tp')
- shared_gate: bfloat16 [512, 2048], P('tp')
- shared_up: bfloat16 [512, 2048], P('tp')
- shared_down: bfloat16 [512, 2048], P('tp')
The draws below stay inside these ranges and needn't reach their ends.
Inputs may be any that keep to these rules, and one draw needn't show every extreme that they name: `routes`: each row names 4 different experts. Among the rows of one device no expert is named by more than 72 rows, and in every draw some expert is named by exactly 72 rows of some device.
All inputs are finite; a program needn't handle non-finite values.
Results may differ from the reference program's by a relative error of at most 0.0085.
Values may be sent and summed in bfloat16 or wider, within the bound.
A program may use at most 64 MiB of HBM per device.

```python
import math
import jax
import jax.numpy as jnp
import numpy as np
from jax import lax

D = 2048
FF_EXPERT = 256
FF_SHARED = 512
TOP = 4
TOK_DEV = 128
EXPERTS = 8
CAP = 72
TOKENS = 4096


def steps_of(own_key, shape, split, smallest, top_value):
    loudness, own = 1.0, jax.random.fold_in(own_key, 6)
    for dim, shards_of in split:
        heights = jnp.exp(jax.random.uniform(jax.random.fold_in(own, dim), (shards_of,), jnp.float32, smallest / len(split), top_value / len(split)))
        loudness = loudness * jnp.repeat(heights, shape[dim] // shards_of).reshape([-1 if axis == dim else 1 for axis in range(len(shape))])
    return loudness


def routed_block(rng, own, number, rows, count, top, most, skew):
    order = jax.random.permutation(rng, count)
    packed, ordinary = load_shares(count, rows * top, most, skew, True), load_shares(count, rows * top, most, skew, False)
    places = jnp.arange(count)

    def named(tallies, turn):
        used = int((tallies > 0).sum())
        fixed = max(1, used // 4)
        passed = fixed + (places - fixed + turn * (used - fixed)) % max(1, count - fixed)
        return jnp.zeros((count,), jnp.int32).at[order[jnp.where(places < fixed, places, passed)]].set(jnp.asarray(tallies, jnp.int32))

    tallies = jnp.where(number % 4 == 0, named(packed, number // 4), named(ordinary, number - number // 4 - 1))
    mixed = jax.random.permutation(jax.random.fold_in(own, 3), count)
    giver, taker = mixed[0:count // 2 * 2:2], mixed[1:count // 2 * 2:2]
    margin = jnp.minimum(tallies[giver] - 1, most - tallies[taker]) // 2
    margin = jnp.where((giver == order[0]) | (taker == order[0]) | (tallies[taker] == 0), 0, jnp.maximum(margin, 0))
    passed = jax.random.randint(jax.random.fold_in(own, 4), (count // 2,), 0, 1 << 20) % (margin + 1)
    tallies = tallies.at[giver].add(-passed).at[taker].add(passed)
    labels = jnp.searchsorted(jnp.cumsum(tallies), jnp.arange(rows * top), side="right").astype(jnp.int32)
    listing = labels.reshape(top, rows).T
    listing = listing[jax.random.permutation(jax.random.fold_in(own, 1), rows)]
    turn = jax.random.randint(jax.random.fold_in(own, 2), (rows, 1), 0, top)
    return jnp.take_along_axis(listing, (jnp.arange(top)[None, :] + turn) % top, axis=1)


def load_shares(number_of, total, bound, skew, full):
    loads = [(1 << 20) // math.isqrt(grade ** skew) + 1 for grade in range(1, number_of + 1)]
    largest = bound if full else min(bound, max(-(-total // number_of), total * loads[0] // sum(loads)))
    least = 1 if total - largest >= number_of - 1 else 0
    given, rest = [largest] + [least] * (number_of - 1), total - largest - least * (number_of - 1)
    while rest > 0:
        movable = [i for i in range(1, number_of) if given[i] < largest] or [i for i in range(1, number_of) if given[i] < bound]
        whole, remaining = sum([loads[i] for i in movable]), rest
        for i in movable:
            more = min(bound - given[i], max(1, remaining * loads[i] // whole), rest)
            given[i] = given[i] + more
            rest = rest - more
    return np.array(given)


def normal_values(key, shape, spread, bound, pieces=(), kind=jnp.bfloat16):
    values = spread * jax.random.normal(key, shape, jnp.float32)
    if pieces:
        values = values * steps_of(key, shape, pieces, -0.22, 0.18)
    return jnp.clip(values, -bound, bound).astype(kind)


def setup_inputs(seed: int = 0) -> dict:
    seeds = jax.random.split(jax.random.key(seed), 11)
    tokens = normal_values(seeds[0], (TOKENS, D), 1.0, 6.0, ((0, 32),))
    gain = jnp.clip(1.0 + 0.18 * jax.random.normal(seeds[1], (D,), jnp.float32), 0.1, 1.9)
    ex_gate = normal_values(seeds[2], (EXPERTS, FF_EXPERT, D), D ** -0.5, 0.125, ((0, 8), (2, 4)), jnp.float32)
    ex_up = normal_values(seeds[3], (EXPERTS, FF_EXPERT, D), D ** -0.5, 0.125, ((0, 8), (2, 4)), jnp.float32)
    ex_down = normal_values(seeds[4], (EXPERTS, FF_EXPERT, D), FF_EXPERT ** -0.5, 0.375, ((0, 8), (2, 4)), jnp.float32)
    sh_gate = normal_values(seeds[5], (FF_SHARED, D), D ** -0.5, 0.125, ((0, 8), (1, 4)), jnp.float32)
    sh_up = normal_values(seeds[6], (FF_SHARED, D), D ** -0.5, 0.125, ((0, 8), (1, 4)), jnp.float32)
    sh_down = normal_values(seeds[7], (FF_SHARED, D), FF_SHARED ** -0.5, 0.25, ((0, 8), (1, 4)), jnp.float32)
    routes_keys = jax.random.split(jax.random.fold_in(seeds[8], 1), TOKENS // TOK_DEV)
    routes_turns = jax.random.permutation(jax.random.fold_in(seeds[8], 3), TOKENS // TOK_DEV)
    routes = jax.vmap(lambda own, number: routed_block(jax.random.fold_in(seeds[8], 2), own, number, TOK_DEV, EXPERTS, TOP, CAP, 2))(routes_keys, routes_turns).reshape((TOKENS, TOP))
    route_weight = jnp.clip(jnp.exp(math.log(1.0) - 2.3025851 * jax.random.uniform(seeds[9], (TOKENS, TOP), jnp.float32) ** steps_of(seeds[9], (TOKENS, TOP), ((0, 32),), -0.2, 0.2)), 0.1, 1.0)
    return {"tokens": tokens, "gain": gain, "ex_gate": ex_gate, "ex_up": ex_up, "ex_down": ex_down, "sh_gate": sh_gate, "sh_up": sh_up, "sh_down": sh_down, "routes": routes, "route_weight": route_weight}


EPS = 1e-06
ROUTED_SCALE = 2.5
CONTRACT = (((1,), (1,)), ((), ()))

def against(row_block, weight):
    return lax.dot_general(row_block, weight, CONTRACT, preferred_element_type=jnp.float32)

def expert_apply(row_block, w_gate, w_up, w_down):
    hidden = (jax.nn.silu(against(row_block, w_gate)) * against(row_block, w_up)).astype(jnp.bfloat16)
    return jnp.dot(hidden, w_down, preferred_element_type=jnp.float32)

def slot_numbers(expert_ids, experts, capacity):
    flat_ids = expert_ids.reshape(-1).astype(jnp.int32)
    onehot = (flat_ids[:, None] == jnp.arange(experts, dtype=jnp.int32)[None, :]).astype(jnp.int32)
    before = jnp.cumsum(onehot, axis=0) - onehot
    ranking = lax.optimization_barrier(jnp.sum(before * onehot, axis=1)).astype(jnp.int32)
    return (flat_ids * capacity + ranking).astype(jnp.int32)

def reference(tokens, gain, ex_gate, ex_up, ex_down, sh_gate, sh_up, sh_down, routes, route_weight):
    scale = gain[None, :]
    expert_gate = (ex_gate * scale[None]).astype(jnp.bfloat16)
    expert_up = (ex_up * scale[None]).astype(jnp.bfloat16)
    expert_down = ex_down.astype(jnp.bfloat16)
    shared_gate = (sh_gate * scale).astype(jnp.bfloat16)
    shared_up = (sh_up * scale).astype(jnp.bfloat16)
    shared_down = sh_down.astype(jnp.bfloat16)
    values = tokens.astype(jnp.float32)
    normed = (values * lax.rsqrt(lax.optimization_barrier(jnp.mean(values * values, axis=1, keepdims=True)) + EPS)).astype(jnp.bfloat16)
    weights = route_weight / lax.optimization_barrier(jnp.sum(route_weight, axis=1, keepdims=True)) * ROUTED_SCALE
    blocks = TOKENS // TOK_DEV
    spots = jnp.arange(EXPERTS * CAP, dtype=jnp.int32)

    def one_block(inputs):
        row_block, expert_ids, block_weights = inputs
        shared = expert_apply(row_block, shared_gate, shared_up, shared_down)
        slots = slot_numbers(expert_ids, EXPERTS, CAP)
        placing = (spots[:, None] == slots[None, :]).astype(jnp.int32)
        placing = lax.optimization_barrier(jnp.sum(placing.reshape(EXPERTS * CAP, TOK_DEV, TOP), axis=2)).astype(jnp.bfloat16)
        outgoing = jnp.dot(placing, row_block, preferred_element_type=jnp.float32).astype(jnp.bfloat16)
        outgoing = outgoing.reshape(EXPERTS, CAP, D)

        def per_expert(parts):
            slot_rows, w_gate, w_up, w_down = parts
            return expert_apply(slot_rows, w_gate, w_up, w_down).astype(jnp.bfloat16)
        answered = lax.map(per_expert, (outgoing, expert_gate, expert_up, expert_down))
        picked = answered.reshape(EXPERTS * CAP, D)[slots].reshape(TOK_DEV, TOP, D)
        routed = lax.optimization_barrier(jnp.sum(block_weights[:, :, None] * picked.astype(jnp.float32), axis=1))
        return (shared + routed).astype(jnp.bfloat16)
    mixed = lax.map(one_block, (normed.reshape(blocks, TOK_DEV, D), routes.reshape(blocks, TOK_DEV, TOP), weights.reshape(blocks, TOK_DEV, TOP)))
    return (mixed.reshape(TOKENS, D), expert_gate, expert_up, expert_down, shared_gate, shared_up, shared_down)
```

```python
import functools

import jax
import jax.numpy as jnp
from jax import lax
from jax.experimental import pallas as pl
from jax.experimental.pallas import tpu as pltpu
from jax.sharding import PartitionSpec as P

EPS = 1e-06
ROUTED_SCALE = 2.5
CONTRACT = (((1,), (1,)), ((), ()))
MESH = pl.DeviceIdType.MESH
LAG = 2
RING = 16


def kernel(
    F, T, H, S, M,
    tokens, gain, ex_gate, ex_up, ex_down, sh_gate, sh_up, sh_down, routes, rweight,
    o_mixed, o_eg, o_eu, o_ed, o_sg, o_su, o_sd,
    tok, wbuf, wt, hid_e, hid_s, own, pout, pin, sout, sin, mix,
    ag_send, ag_recv, wt_send, wt_recv, w_send, w_recv,
    pout_sem, pin_sem, sout_sem, sin_sem, out_sem, mix_sem,
):
    f = lax.axis_index("fs")
    me = lax.axis_index("tp")
    z = me // 2
    c = lax.rem(me, 2)
    Z = T // 2
    cw = wbuf.shape[2]
    rows = tokens.shape[0]
    GU = 2 * H + 2 * S
    ALL = 3 * H + 3 * S
    partner = 2 * z + 1 - c

    barrier = pltpu.get_barrier_semaphore()
    for i in range(1, F):
        pl.semaphore_signal(barrier, inc=1, device_id=(lax.rem(f + i, F), me), device_id_type=MESH)
    for i in range(1, T):
        pl.semaphore_signal(barrier, inc=1, device_id=(f, lax.rem(me + i, T)), device_id_type=MESH)

    scale = gain[...]
    values = tokens[...].astype(jnp.float32)
    inv = lax.rsqrt(jnp.mean(values * values, axis=1, keepdims=True) + EPS)
    tok[me] = (values * inv).astype(jnp.bfloat16)
    wbuf[f, 0:H, :] = (ex_gate[...] * scale).astype(jnp.bfloat16)
    wbuf[f, H:2 * H, :] = (ex_up[...] * scale).astype(jnp.bfloat16)
    wbuf[f, 2 * H:2 * H + S, :] = (sh_gate[...] * scale).astype(jnp.bfloat16)
    wbuf[f, 2 * H + S:GU, :] = (sh_up[...] * scale).astype(jnp.bfloat16)
    wbuf[f, GU:GU + H, :] = ex_down[...].astype(jnp.bfloat16)
    wbuf[f, GU + H:ALL, :] = sh_down[...].astype(jnp.bfloat16)
    rw = rweight[...]
    w = rw / jnp.sum(rw, axis=1, keepdims=True) * ROUTED_SCALE
    ids = routes[...]
    lane = lax.broadcasted_iota(jnp.int32, (rows, 128), 1)
    comb = jnp.zeros((rows, 128), jnp.float32)
    for k in range(ids.shape[1]):
        comb = comb + jnp.where(lane == ids[:, k:k + 1], w[:, k:k + 1], 0.0)
    wt[me] = jnp.transpose(comb)[:T, :]

    pl.semaphore_wait(barrier, F - 1 + T - 1)

    def rdma(src, dst, ssem, rsem, dev):
        return pltpu.make_async_remote_copy(
            src_ref=src, dst_ref=dst, send_sem=ssem, recv_sem=rsem,
            device_id=dev, device_id_type=MESH,
        )

    def tok_copy(s, way, t):
        return rdma(tok.at[s], tok.at[s], ag_send.at[s, way], ag_recv.at[s], (f, t))

    def w_copy(part, src, i, peer):
        lo, hi = ((0, GU), (GU, ALL))[part]
        return rdma(
            wbuf.at[src, lo:hi, :], wbuf.at[src, lo:hi, :],
            w_send.at[part, i], w_recv.at[part, src], (peer, me),
        )

    def wt_copy(s, i, t):
        return rdma(wt.at[s], wt.at[s], wt_send.at[i], wt_recv.at[s], (f, t))

    def right(t):
        return jnp.minimum(t + 2, T - 2 + lax.rem(t, 2))

    def left(t):
        return jnp.maximum(t - 2, lax.rem(t, 2))

    @pl.when(z < Z - 1)
    def _():
        tok_copy(me, 0, right(me)).start()

    @pl.when(z > 0)
    def _():
        tok_copy(me, 1, left(me)).start()

    for i in range(1, F):
        w_copy(0, f, i, lax.rem(f + i, F)).start()
    tok_copy(me, 2, partner).start()
    for i in range(1, T):
        wt_copy(me, i, lax.rem(me + i, T)).start()
    for i in range(1, F):
        w_copy(1, f, i, lax.rem(f + i, F)).start()

    def gather_step(k, carry):
        a = me - 2 * k
        b = me + 2 * k

        @pl.when(a >= 0)
        def _():
            tok_copy(a, 0, partner).wait_recv()

            @pl.when(z < Z - 1)
            def _():
                tok_copy(a, 0, right(me)).start()

            tok_copy(a, 2, partner).start()

        @pl.when(b < T)
        def _():
            tok_copy(b, 1, partner).wait_recv()

            @pl.when(z > 0)
            def _():
                tok_copy(b, 1, left(me)).start()

            tok_copy(b, 2, partner).start()

        return carry

    lax.fori_loop(1, Z, gather_step, 0)

    for i in range(1, F):
        w_copy(0, lax.rem(f + F - i, F), i, f).wait_recv()
    for i in range(1, T):
        wt_copy(lax.rem(me + T - i, T), i, me).wait_recv()

    pieces = ((o_eg, 0, H), (o_eu, H, H), (o_sg, 2 * H, S), (o_su, 2 * H + S, S), (o_ed, GU, H), (o_sd, GU + H, S))

    def out_copy(p, q):
        ref, lo, size = pieces[p]
        return pltpu.make_async_copy(
            wbuf.at[q, lo:lo + size, :], ref.at[:, q * cw:(q + 1) * cw], out_sem.at[p, q]
        )

    for p in range(4):
        for q in range(F):
            out_copy(p, q).start()

    def hidden_step(k, carry):
        tok_copy(2 * k + 1 - c, 0, partner).wait_recv()
        x = tok[pl.ds(2 * k, 2)].reshape(2 * rows, F * cw)
        acc = jnp.zeros((2 * rows, GU), jnp.float32)
        for q in range(F):
            acc = acc + lax.dot_general(
                x[:, q * cw:(q + 1) * cw], wbuf[q, 0:GU, :], CONTRACT,
                preferred_element_type=jnp.float32,
            )
        g, u = acc[:, 0:H], acc[:, H:2 * H]
        sg, su = acc[:, 2 * H:2 * H + S], acc[:, 2 * H + S:GU]
        he = g / (1.0 + jnp.exp(-g)) * u
        hs = sg / (1.0 + jnp.exp(-sg)) * su
        for h in range(2):
            row = wt[2 * k + h, pl.ds(me, 1), :]
            col = jnp.transpose(jnp.broadcast_to(row, (128, rows)))[:, 0:1]
            hid_e[2 * k + h] = (he[h * rows:(h + 1) * rows] * col).astype(jnp.bfloat16)
            hid_s[2 * k + h] = hs[h * rows:(h + 1) * rows].astype(jnp.bfloat16)
        return carry

    lax.fori_loop(0, Z, hidden_step, 0)

    N = (Z - 1) * F
    U = Z * F
    ring = pout.shape[0]
    spot = jnp.where(2 * z >= Z, 2 * (Z - 1 - z), 2 * z + 1)

    def unit(u):
        i = lax.rem(u, Z - 1)
        i = i + jnp.where(i >= spot, 1, 0)
        d = jnp.where(lax.rem(i, 2) == 0, Z - 1 - i // 2, i // 2)
        j = u // (Z - 1)
        d = jnp.where(u < N, d, z)
        j = jnp.where(u < N, j, u - N)
        return j, d

    def pair_copy(u):
        p = lax.rem(u, ring)
        return rdma(pout.at[p], pin.at[u], pout_sem.at[p], pin_sem.at[u], (f, partner))

    def sum_copy(u, slot, t):
        p = lax.rem(u, ring)
        return rdma(sout.at[p], sin.at[slot], sout_sem.at[p], sin_sem.at[slot], (f, t))

    def mix_copy(q):
        return pltpu.make_async_copy(
            mix.at[q], o_mixed.at[:, pl.ds(pl.multiple_of(q * cw, 128), cw)], mix_sem.at[q]
        )

    def produce(u):
        j, d = unit(u)
        q = lax.rem(f + j, F)

        @pl.when((j > 0) & (lax.rem(u, Z - 1) == 0) & (u < N))
        def _():
            w_copy(1, q, 1, f).wait_recv()

        he = hid_e[pl.ds(2 * d, 2)].reshape(2 * rows, H)
        hs = hid_s[pl.ds(2 * d, 2)].reshape(2 * rows, S)
        r = jnp.dot(he, wbuf[q, GU:GU + H, :], preferred_element_type=jnp.float32)
        r = r + jnp.dot(hs, wbuf[q, GU + H:ALL, :], preferred_element_type=jnp.float32)
        top, bottom = r[:rows], r[rows:]
        own[lax.rem(u, LAG + 1)] = jnp.where(c == 0, top, bottom)

        @pl.when(u >= ring)
        def _():
            pair_copy(u - ring).wait_send()

        pout[lax.rem(u, ring)] = jnp.where(c == 0, bottom, top).astype(jnp.bfloat16)
        pair_copy(u).start()

    def finish(u):
        j, d = unit(u)
        q = lax.rem(f + j, F)
        o = lax.rem(u, LAG + 1)
        from_left = (d >= z) & (z > 0)
        from_right = (d <= z) & (z < Z - 1)
        pair_copy(u).wait_recv()
        own[o] = own[o] + pin[u].astype(jnp.float32)
        base = j * (Z + 1)

        @pl.when(from_left)
        def _():
            sum_copy(u, base + d, me).wait_recv()
            own[o] = own[o] + sin[base + d].astype(jnp.float32)

        @pl.when(from_right)
        def _():
            slot = base + jnp.where(d == z, Z, d)
            sum_copy(u, slot, me).wait_recv()
            own[o] = own[o] + sin[slot].astype(jnp.float32)

        @pl.when(u < N)
        def _():
            @pl.when(u >= ring)
            def _():
                sum_copy(u - ring, 0, partner).wait_send()

            sout[lax.rem(u, ring)] = own[o].astype(jnp.bfloat16)

            @pl.when(d > z)
            def _():
                sum_copy(u, base + d, right(me)).start()

            @pl.when(d < z)
            def _():
                sum_copy(u, base + jnp.where(d == z - 1, Z, d), left(me)).start()

        @pl.when(u >= N)
        def _():
            mix[q] = own[o].astype(jnp.bfloat16)
            mix_copy(q).start()

    def sum_step(u, carry):
        @pl.when(u < U)
        def _():
            produce(u)

        @pl.when(u >= LAG)
        def _():
            finish(u - LAG)

        return carry

    lax.fori_loop(0, U + LAG, sum_step, 0)

    for p in range(4, 6):
        for q in range(F):
            out_copy(p, q).start()
    for u in range(max(0, U - ring), U):
        pair_copy(u).wait_send()
    for u in range(max(0, N - ring), N):
        sum_copy(u, 0, partner).wait_send()
    for i in range(1, F):
        w_copy(0, f, i, lax.rem(f + i, F)).wait_send()
        w_copy(1, f, i, lax.rem(f + i, F)).wait_send()
    for i in range(1, T):
        wt_copy(me, i, lax.rem(me + i, T)).wait_send()

    def drain(k, carry):
        s = 2 * k + c

        @pl.when((k <= z) & (z < Z - 1))
        def _():
            tok_copy(s, 0, right(me)).wait_send()

        @pl.when((k >= z) & (z > 0))
        def _():
            tok_copy(s, 1, left(me)).wait_send()

        tok_copy(s, 2, partner).wait_send()
        return carry

    lax.fori_loop(0, Z, drain, 0)
    for q in range(F):
        mix_copy(q).wait()
    for p in range(6):
        for q in range(F):
            out_copy(p, q).wait()


def local(F, T, tokens, gain, ex_gate, ex_up, ex_down, sh_gate, sh_up, sh_down, routes, route_weight):
    H, cw = ex_gate.shape[1:]
    S = sh_gate.shape[0]
    M = tokens.shape[0]
    D = tokens.shape[1]
    Z = T // 2
    N, U = (Z - 1) * F, Z * F
    ring = min(U, RING)
    bf, f32 = jnp.bfloat16, jnp.float32
    dma = pltpu.SemaphoreType.DMA
    out = pl.pallas_call(
        functools.partial(kernel, F, T, H, S, M),
        out_shape=[jax.ShapeDtypeStruct((M, D), bf)]
        + [jax.ShapeDtypeStruct((H, D), bf)] * 3
        + [jax.ShapeDtypeStruct((S, D), bf)] * 3,
        in_specs=[pl.BlockSpec(memory_space=pltpu.VMEM)] * 10,
        out_specs=[pl.BlockSpec(memory_space=pl.ANY)] * 7,
        scratch_shapes=[
            pltpu.VMEM((T, M, D), bf),
            pltpu.VMEM((F, 3 * H + 3 * S, cw), bf),
            pltpu.VMEM((T, T, M), f32),
            pltpu.VMEM((T, M, H), bf),
            pltpu.VMEM((T, M, S), bf),
            pltpu.VMEM((LAG + 1, M, cw), f32),
            pltpu.VMEM((ring, M, cw), bf),
            pltpu.VMEM((U, M, cw), bf),
            pltpu.VMEM((ring, M, cw), bf),
            pltpu.VMEM((F * (Z + 1), M, cw), bf),
            pltpu.VMEM((F, M, cw), bf),
            dma((T, 3)),
            dma((T,)),
            dma((T,)),
            dma((T,)),
            dma((2, F)),
            dma((2, F)),
            dma((ring,)),
            dma((U,)),
            dma((ring,)),
            dma((F * (Z + 1),)),
            dma((6, F)),
            dma((F,)),
        ],
        compiler_params=pltpu.CompilerParams(
            collective_id=0, has_side_effects=True, vmem_limit_bytes=67043328
        ),
    )(
        tokens, gain[None, :], ex_gate[0], ex_up[0], ex_down[0], sh_gate, sh_up, sh_down,
        routes, route_weight,
    )
    mixed, eg, eu, ed, sg, su, sd = out
    return (mixed, eg[None], eu[None], ed[None], sg, su, sd)


def solution(mesh):
    in_specs = (
        P(("fs", "tp"), None),
        P("fs"),
        P("tp", None, "fs"),
        P("tp", None, "fs"),
        P("tp", None, "fs"),
        P("tp", "fs"),
        P("tp", "fs"),
        P("tp", "fs"),
        P(("fs", "tp"), None),
        P(("fs", "tp"), None),
    )
    out_specs = (
        P(("fs", "tp"), None),
        P("tp", None, None),
        P("tp", None, None),
        P("tp", None, None),
        P("tp", None),
        P("tp", None),
        P("tp", None),
    )
    step = functools.partial(local, mesh.shape["fs"], mesh.shape["tp"])
    return jax.shard_map(step, mesh=mesh, in_specs=in_specs, out_specs=out_specs, check_vma=False)
```

```python
import functools

import jax
import jax.numpy as jnp
from jax import lax
from jax.experimental import pallas as pl
from jax.experimental.pallas import tpu as pltpu
from jax.sharding import PartitionSpec as P

EPS = 1e-06
ROUTED_SCALE = 2.5
CONTRACT = (((1,), (1,)), ((), ()))
MESH = pl.DeviceIdType.MESH
LAG = 2
RING = 16
VMEM_LIMIT = 56 << 20


def kernel(
    F, T, H, S, M,
    tokens, gain, ex_gate, ex_up, ex_down, sh_gate, sh_up, sh_down, routes, rweight,
    wbuf, mix,
    tok, wt, hid_e, hid_s, own, pout, pin, sout, sin,
    ag_send, ag_recv, wt_send, wt_recv, w_send, w_recv,
    pout_sem, pin_sem, sout_sem, sin_sem,
):
    f = lax.axis_index("fs")
    me = lax.axis_index("tp")
    z = me // 2
    c = lax.rem(me, 2)
    Z = T // 2
    cw = wbuf.shape[2]
    rows = tokens.shape[0]
    GU = 2 * H + 2 * S
    ALL = 3 * H + 3 * S
    partner = 2 * z + 1 - c

    barrier = pltpu.get_barrier_semaphore()
    for i in range(1, F):
        pl.semaphore_signal(barrier, inc=1, device_id=(lax.rem(f + i, F), me), device_id_type=MESH)
    for i in range(1, T):
        pl.semaphore_signal(barrier, inc=1, device_id=(f, lax.rem(me + i, T)), device_id_type=MESH)

    values = tokens[...].astype(jnp.float32)
    inv = lax.rsqrt(jnp.mean(values * values, axis=1, keepdims=True) + EPS)
    tok[me] = (values * inv).astype(jnp.bfloat16)
    rw = rweight[...]
    w = rw / jnp.sum(rw, axis=0, keepdims=True) * ROUTED_SCALE
    ids = routes[...]
    expert = lax.broadcasted_iota(jnp.int32, (T, rows), 0)
    comb = jnp.zeros((T, rows), jnp.float32)
    for k in range(ids.shape[0]):
        comb = comb + jnp.where(expert == ids[k:k + 1, :], w[k:k + 1, :], 0.0)
    wt[me] = comb

    pl.semaphore_wait(barrier, F - 1 + T - 1)

    def rdma(src, dst, ssem, rsem, dev):
        return pltpu.make_async_remote_copy(
            src_ref=src, dst_ref=dst, send_sem=ssem, recv_sem=rsem,
            device_id=dev, device_id_type=MESH,
        )

    def tok_copy(s, way, t):
        return rdma(tok.at[s], tok.at[s], ag_send.at[s, way], ag_recv.at[s], (f, t))

    def w_copy(part, src, i, peer):
        lo, hi = ((0, GU), (GU, ALL))[part]
        return rdma(
            wbuf.at[src, lo:hi, :], wbuf.at[src, lo:hi, :],
            w_send.at[part, i], w_recv.at[part, src], (peer, me),
        )

    def wt_copy(s, i, t):
        return rdma(wt.at[s], wt.at[s], wt_send.at[i], wt_recv.at[s], (f, t))

    def right(t):
        return jnp.minimum(t + 2, T - 2 + lax.rem(t, 2))

    def left(t):
        return jnp.maximum(t - 2, lax.rem(t, 2))

    @pl.when(z < Z - 1)
    def _():
        tok_copy(me, 0, right(me)).start()

    @pl.when(z > 0)
    def _():
        tok_copy(me, 1, left(me)).start()

    tok_copy(me, 2, partner).start()
    for i in range(1, T):
        wt_copy(me, i, lax.rem(me + i, T)).start()
    scale = gain[...]
    wbuf[f, 0:H, :] = (ex_gate[...] * scale).astype(jnp.bfloat16)
    wbuf[f, H:2 * H, :] = (ex_up[...] * scale).astype(jnp.bfloat16)
    wbuf[f, 2 * H:2 * H + S, :] = (sh_gate[...] * scale).astype(jnp.bfloat16)
    wbuf[f, 2 * H + S:GU, :] = (sh_up[...] * scale).astype(jnp.bfloat16)
    wbuf[f, GU:GU + H, :] = ex_down[...].astype(jnp.bfloat16)
    wbuf[f, GU + H:ALL, :] = sh_down[...].astype(jnp.bfloat16)
    for i in range(1, F):
        w_copy(0, f, i, lax.rem(f + i, F)).start()
    for i in range(1, F):
        w_copy(1, f, i, lax.rem(f + i, F)).start()

    def gather_step(k, carry):
        a = me - 2 * k
        b = me + 2 * k

        @pl.when(a >= 0)
        def _():
            tok_copy(a, 0, partner).wait_recv()

            @pl.when(z < Z - 1)
            def _():
                tok_copy(a, 0, right(me)).start()

            tok_copy(a, 2, partner).start()

        @pl.when(b < T)
        def _():
            tok_copy(b, 1, partner).wait_recv()

            @pl.when(z > 0)
            def _():
                tok_copy(b, 1, left(me)).start()

            tok_copy(b, 2, partner).start()

        return carry

    lax.fori_loop(1, Z - 1, gather_step, 0)

    for i in range(1, F):
        w_copy(0, lax.rem(f + F - i, F), i, f).wait_recv()
    for i in range(1, T):
        wt_copy(lax.rem(me + T - i, T), i, me).wait_recv()

    def hidden_step(k, carry):
        tok_copy(2 * k + 1 - c, 0, partner).wait_recv()
        x = tok[pl.ds(2 * k, 2)].reshape(2 * rows, F * cw)
        acc = jnp.zeros((2 * rows, GU), jnp.float32)
        for q in range(F):
            acc = acc + lax.dot_general(
                x[:, q * cw:(q + 1) * cw], wbuf[q, 0:GU, :], CONTRACT,
                preferred_element_type=jnp.float32,
            )
        g, u = acc[:, 0:H], acc[:, H:2 * H]
        sg, su = acc[:, 2 * H:2 * H + S], acc[:, 2 * H + S:GU]
        he = g / (1.0 + jnp.exp(-g)) * u
        hs = sg / (1.0 + jnp.exp(-sg)) * su
        for h in range(2):
            row = wt[2 * k + h, pl.ds(me, 1), :]
            col = jnp.transpose(jnp.broadcast_to(row, (128, rows)))[:, 0:1]
            hid_e[2 * k + h] = (he[h * rows:(h + 1) * rows] * col).astype(jnp.bfloat16)
            hid_s[2 * k + h] = hs[h * rows:(h + 1) * rows].astype(jnp.bfloat16)
        return carry

    def near_step(k, carry):
        @pl.when(jnp.maximum(k - z, z - k) < Z - 1)
        def _():
            hidden_step(k, carry)

        return carry

    lax.fori_loop(0, Z, near_step, 0)
    gather_step(Z - 1, 0)

    @pl.when(z == 0)
    def _():
        hidden_step(Z - 1, 0)

    @pl.when(z == Z - 1)
    def _():
        hidden_step(0, 0)

    ring = pout.shape[0]
    big = Z * F
    near = jnp.minimum(jnp.where(z < Z - 1, z, big), jnp.where(z > 0, Z - 1 - z, big))
    count = Z * (F + Z - 1)

    def unit(n):
        s = n // Z
        i = lax.rem(n, Z)
        d = jnp.where(lax.rem(i, 2) == 0, Z - 1 - i // 2, i // 2)
        away = jnp.where(d > z, z, jnp.where(d < z, Z - 1 - z, jnp.maximum(z, Z - 1 - z)))
        j = s - away
        return j, d, (j >= 0) & (j < F) & (n >= 0) & (n < count)

    def pair_copy(p, slot):
        return rdma(pout.at[p], pin.at[slot], pout_sem.at[p], pin_sem.at[slot], (f, partner))

    def sum_copy(p, slot, t):
        return rdma(sout.at[p], sin.at[slot], sout_sem.at[p], sin_sem.at[slot], (f, t))

    def produce(n, j, d, done):
        q = lax.rem(f + j, F)
        p = lax.rem(done, ring)
        he = hid_e[pl.ds(2 * d, 2)].reshape(2 * rows, H)
        hs = hid_s[pl.ds(2 * d, 2)].reshape(2 * rows, S)
        r = jnp.dot(he, wbuf[q, GU:GU + H, :], preferred_element_type=jnp.float32)
        r = r + jnp.dot(hs, wbuf[q, GU + H:ALL, :], preferred_element_type=jnp.float32)
        top, bottom = r[:rows], r[rows:]
        own[lax.rem(n, LAG + 1)] = jnp.where(c == 0, top, bottom)

        @pl.when(done >= ring)
        def _():
            pair_copy(p, 0).wait_send()

        pout[p] = jnp.where(c == 0, bottom, top).astype(jnp.bfloat16)
        pair_copy(p, j * Z + d).start()

    def finish(n, j, d, sent):
        q = lax.rem(f + j, F)
        o = lax.rem(n, LAG + 1)
        p = lax.rem(sent, ring)
        base = j * (Z + 1)
        pair_copy(0, j * Z + d).wait_recv()
        own[o] = own[o] + pin[j * Z + d].astype(jnp.float32)

        @pl.when((d >= z) & (z > 0))
        def _():
            sum_copy(0, base + d, me).wait_recv()
            own[o] = own[o] + sin[base + d].astype(jnp.float32)

        @pl.when((d <= z) & (z < Z - 1))
        def _():
            slot = base + jnp.where(d == z, Z, d)
            sum_copy(0, slot, me).wait_recv()
            own[o] = own[o] + sin[slot].astype(jnp.float32)

        @pl.when(d != z)
        def _():
            @pl.when(sent >= ring)
            def _():
                sum_copy(p, 0, partner).wait_send()

            sout[p] = own[o].astype(jnp.bfloat16)

            @pl.when(d > z)
            def _():
                sum_copy(p, base + d, right(me)).start()

            @pl.when(d < z)
            def _():
                sum_copy(p, base + jnp.where(d == z - 1, Z, d), left(me)).start()

        @pl.when(d == z)
        def _():
            mix[q] = own[o].astype(jnp.bfloat16)

    def sum_step(n, carry):
        done, sent = carry
        first = n // Z - near

        @pl.when((lax.rem(n, Z) == 0) & (first > 0) & (first < F))
        def _():
            w_copy(1, lax.rem(f + first, F), 1, f).wait_recv()

        j, d, valid = unit(n)

        @pl.when(valid)
        def _():
            produce(n, j, d, done)

        done = done + jnp.where(valid, 1, 0)
        m = n - LAG
        j, d, valid = unit(jnp.maximum(m, 0))
        valid = valid & (m >= 0)

        @pl.when(valid)
        def _():
            finish(m, j, d, sent)

        sent = sent + jnp.where(valid & (d != z), 1, 0)
        return done, sent

    lax.fori_loop(0, count + LAG, sum_step, (0, 0))

    for p in range(ring):
        pair_copy(p, 0).wait_send()
    for p in range(min(ring, (Z - 1) * F)):
        sum_copy(p, 0, partner).wait_send()
    for i in range(1, F):
        w_copy(0, f, i, lax.rem(f + i, F)).wait_send()
        w_copy(1, f, i, lax.rem(f + i, F)).wait_send()
    for i in range(1, T):
        wt_copy(me, i, lax.rem(me + i, T)).wait_send()

    def drain(k, carry):
        s = 2 * k + c

        @pl.when((k <= z) & (z < Z - 1))
        def _():
            tok_copy(s, 0, right(me)).wait_send()

        @pl.when((k >= z) & (z > 0))
        def _():
            tok_copy(s, 1, left(me)).wait_send()

        tok_copy(s, 2, partner).wait_send()
        return carry

    lax.fori_loop(0, Z, drain, 0)


def place(H, S, wbuf, mix, o_mixed, o_eg, o_eu, o_ed, o_sg, o_su, o_sd, sems):
    F, cw = wbuf.shape[0], wbuf.shape[2]
    GU = 2 * H + 2 * S
    pieces = ((o_eg, 0, H), (o_eu, H, H), (o_ed, GU, H), (o_sg, 2 * H, S), (o_su, 2 * H + S, S), (o_sd, GU + H, S))
    copies = []
    for p, (ref, lo, size) in enumerate(pieces):
        for q in range(F):
            copies.append(pltpu.make_async_copy(
                wbuf.at[q, lo:lo + size, :], ref.at[:, q * cw:(q + 1) * cw], sems.at[p, q]
            ))
    for q in range(F):
        copies.append(pltpu.make_async_copy(mix.at[q], o_mixed.at[:, q * cw:(q + 1) * cw], sems.at[6, q]))
    for copy in copies:
        copy.start()
    for copy in copies:
        copy.wait()


def local(F, T, tokens, gain, ex_gate, ex_up, ex_down, sh_gate, sh_up, sh_down, routes, route_weight):
    H, cw = ex_gate.shape[1:]
    S = sh_gate.shape[0]
    M = tokens.shape[0]
    D = tokens.shape[1]
    Z = T // 2
    N, U = (Z - 1) * F, Z * F
    ring = min(U, RING)
    bf, f32 = jnp.bfloat16, jnp.float32
    dma = pltpu.SemaphoreType.DMA
    wbuf, mix = pl.pallas_call(
        functools.partial(kernel, F, T, H, S, M),
        out_shape=[pltpu.VMEM((F, 3 * H + 3 * S, cw), bf), pltpu.VMEM((F, M, cw), bf)],
        in_specs=[pl.BlockSpec(memory_space=pltpu.VMEM)] * 10,
        out_specs=[pl.BlockSpec(memory_space=pltpu.VMEM)] * 2,
        scratch_shapes=[
            pltpu.VMEM((T, M, D), bf),
            pltpu.VMEM((T, T, M), f32),
            pltpu.VMEM((T, M, H), bf),
            pltpu.VMEM((T, M, S), bf),
            pltpu.VMEM((LAG + 1, M, cw), f32),
            pltpu.VMEM((ring, M, cw), bf),
            pltpu.VMEM((U, M, cw), bf),
            pltpu.VMEM((ring, M, cw), bf),
            pltpu.VMEM((F * (Z + 1), M, cw), bf),
            dma((T, 3)),
            dma((T,)),
            dma((T,)),
            dma((T,)),
            dma((2, F)),
            dma((2, F)),
            dma((ring,)),
            dma((U,)),
            dma((ring,)),
            dma((F * (Z + 1),)),
        ],
        compiler_params=pltpu.CompilerParams(
            collective_id=0, has_side_effects=True, vmem_limit_bytes=VMEM_LIMIT
        ),
    )(
        tokens, gain[None, :], ex_gate[0], ex_up[0], ex_down[0], sh_gate, sh_up, sh_down,
        routes.T, route_weight.T,
    )
    mixed, eg, eu, ed, sg, su, sd = pl.pallas_call(
        functools.partial(place, H, S),
        out_shape=[jax.ShapeDtypeStruct((M, D), bf)]
        + [jax.ShapeDtypeStruct((H, D), bf)] * 3
        + [jax.ShapeDtypeStruct((S, D), bf)] * 3,
        in_specs=[pl.BlockSpec(memory_space=pltpu.VMEM)] * 2,
        out_specs=[pl.BlockSpec(memory_space=pl.ANY)] * 7,
        scratch_shapes=[dma((7, F))],
        compiler_params=pltpu.CompilerParams(vmem_limit_bytes=4 << 20),
    )(pltpu.with_memory_space_constraint(wbuf, pltpu.VMEM), pltpu.with_memory_space_constraint(mix, pltpu.VMEM))
    return (mixed, eg[None], eu[None], ed[None], sg, su, sd)


def solution(mesh):
    in_specs = (
        P(("fs", "tp"), None),
        P("fs"),
        P("tp", None, "fs"),
        P("tp", None, "fs"),
        P("tp", None, "fs"),
        P("tp", "fs"),
        P("tp", "fs"),
        P("tp", "fs"),
        P(("fs", "tp"), None),
        P(("fs", "tp"), None),
    )
    out_specs = (
        P(("fs", "tp"), None),
        P("tp", None, None),
        P("tp", None, None),
        P("tp", None, None),
        P("tp", None),
        P("tp", None),
        P("tp", None),
    )
    step = functools.partial(local, mesh.shape["fs"], mesh.shape["tp"])
    return jax.shard_map(step, mesh=mesh, in_specs=in_specs, out_specs=out_specs, check_vma=False)
```

```python
import functools

import jax
import jax.numpy as jnp
from jax import lax
from jax.experimental import pallas as pl
from jax.experimental.pallas import tpu as pltpu
from jax.sharding import PartitionSpec as P

EPS = 1e-06
ROUTED_SCALE = 2.5
CONTRACT = (((1,), (1,)), ((), ()))
MESH = pl.DeviceIdType.MESH
LAG = 2
RING = 16
VMEM_LIMIT = 56 << 20


def kernel(
    F, T, H, S, M,
    tokens, gain, ex_gate, ex_up, ex_down, sh_gate, sh_up, sh_down, routes, rweight,
    wbuf, mix,
    tok, wt, hid_e, hid_s, own, pout, pin, sout, sin,
    ag_send, ag_recv, wt_send, wt_recv, w_send, w_recv,
    pout_sem, pin_sem, sout_sem, sin_sem,
    l_eg, l_eu, l_ed, l_sg, l_su, l_sd, load_sem,
):
    f = lax.axis_index("fs")
    me = lax.axis_index("tp")
    z = me // 2
    c = lax.rem(me, 2)
    Z = T // 2
    cw = wbuf.shape[2]
    rows = tokens.shape[0]
    GU = 2 * H + 2 * S
    ALL = 3 * H + 3 * S
    partner = 2 * z + 1 - c

    loads = [
        pltpu.make_async_copy(src, dst, load_sem.at[i])
        for i, (src, dst) in enumerate((
            (ex_gate, l_eg), (ex_up, l_eu), (sh_gate, l_sg), (sh_up, l_su), (ex_down, l_ed), (sh_down, l_sd)
        ))
    ]
    for load in loads:
        load.start()
    barrier = pltpu.get_barrier_semaphore()
    for i in range(1, F):
        pl.semaphore_signal(barrier, inc=1, device_id=(lax.rem(f + i, F), me), device_id_type=MESH)
    for i in range(1, T):
        pl.semaphore_signal(barrier, inc=1, device_id=(f, lax.rem(me + i, T)), device_id_type=MESH)

    values = tokens[...].astype(jnp.float32)
    inv = lax.rsqrt(jnp.mean(values * values, axis=1, keepdims=True) + EPS)
    tok[me] = (values * inv).astype(jnp.bfloat16)
    rw = rweight[...]
    w = rw / jnp.sum(rw, axis=0, keepdims=True) * ROUTED_SCALE
    ids = routes[...]
    expert = lax.broadcasted_iota(jnp.int32, (T, rows), 0)
    comb = jnp.zeros((T, rows), jnp.float32)
    for k in range(ids.shape[0]):
        comb = comb + jnp.where(expert == ids[k:k + 1, :], w[k:k + 1, :], 0.0)
    wt[me] = comb

    pl.semaphore_wait(barrier, F - 1 + T - 1)

    def rdma(src, dst, ssem, rsem, dev):
        return pltpu.make_async_remote_copy(
            src_ref=src, dst_ref=dst, send_sem=ssem, recv_sem=rsem,
            device_id=dev, device_id_type=MESH,
        )

    def tok_copy(s, way, t):
        return rdma(tok.at[s], tok.at[s], ag_send.at[s, way], ag_recv.at[s], (f, t))

    def w_copy(part, src, i, peer):
        lo, hi = ((0, GU), (GU, ALL))[part]
        return rdma(
            wbuf.at[src, lo:hi, :], wbuf.at[src, lo:hi, :],
            w_send.at[part, i], w_recv.at[part, src], (peer, me),
        )

    def wt_copy(s, i, t):
        return rdma(wt.at[s], wt.at[s], wt_send.at[i], wt_recv.at[s], (f, t))

    def right(t):
        return jnp.minimum(t + 2, T - 2 + lax.rem(t, 2))

    def left(t):
        return jnp.maximum(t - 2, lax.rem(t, 2))

    @pl.when(z < Z - 1)
    def _():
        tok_copy(me, 0, right(me)).start()

    @pl.when(z > 0)
    def _():
        tok_copy(me, 1, left(me)).start()

    tok_copy(me, 2, partner).start()
    for i in range(1, T):
        wt_copy(me, i, lax.rem(me + i, T)).start()
    for load in loads:
        load.wait()
    scale = gain[...]
    wbuf[f, 0:H, :] = (l_eg[...] * scale).astype(jnp.bfloat16)
    wbuf[f, H:2 * H, :] = (l_eu[...] * scale).astype(jnp.bfloat16)
    wbuf[f, 2 * H:2 * H + S, :] = (l_sg[...] * scale).astype(jnp.bfloat16)
    wbuf[f, 2 * H + S:GU, :] = (l_su[...] * scale).astype(jnp.bfloat16)
    wbuf[f, GU:GU + H, :] = l_ed[...].astype(jnp.bfloat16)
    wbuf[f, GU + H:ALL, :] = l_sd[...].astype(jnp.bfloat16)
    for i in range(1, F):
        w_copy(0, f, i, lax.rem(f + i, F)).start()
    for i in range(1, F):
        w_copy(1, f, i, lax.rem(f + i, F)).start()

    def gather_step(k, carry):
        a = me - 2 * k
        b = me + 2 * k

        @pl.when(a >= 0)
        def _():
            tok_copy(a, 0, partner).wait_recv()

            @pl.when(z < Z - 1)
            def _():
                tok_copy(a, 0, right(me)).start()

            tok_copy(a, 2, partner).start()

        @pl.when(b < T)
        def _():
            tok_copy(b, 1, partner).wait_recv()

            @pl.when(z > 0)
            def _():
                tok_copy(b, 1, left(me)).start()

            tok_copy(b, 2, partner).start()

        return carry

    lax.fori_loop(1, Z - 1, gather_step, 0)

    for i in range(1, F):
        w_copy(0, lax.rem(f + F - i, F), i, f).wait_recv()
    for i in range(1, T):
        wt_copy(lax.rem(me + T - i, T), i, me).wait_recv()

    def hidden_step(k, carry):
        tok_copy(2 * k + 1 - c, 0, partner).wait_recv()
        x = tok[pl.ds(2 * k, 2)].reshape(2 * rows, F * cw)
        acc = jnp.zeros((2 * rows, GU), jnp.float32)
        for q in range(F):
            acc = acc + lax.dot_general(
                x[:, q * cw:(q + 1) * cw], wbuf[q, 0:GU, :], CONTRACT,
                preferred_element_type=jnp.float32,
            )
        g, u = acc[:, 0:H], acc[:, H:2 * H]
        sg, su = acc[:, 2 * H:2 * H + S], acc[:, 2 * H + S:GU]
        he = g / (1.0 + jnp.exp(-g)) * u
        hs = sg / (1.0 + jnp.exp(-sg)) * su
        for h in range(2):
            row = wt[2 * k + h, pl.ds(me, 1), :]
            col = jnp.transpose(jnp.broadcast_to(row, (128, rows)))[:, 0:1]
            hid_e[2 * k + h] = (he[h * rows:(h + 1) * rows] * col).astype(jnp.bfloat16)
            hid_s[2 * k + h] = hs[h * rows:(h + 1) * rows].astype(jnp.bfloat16)
        return carry

    def near_step(k, carry):
        @pl.when(jnp.maximum(k - z, z - k) < Z - 1)
        def _():
            hidden_step(k, carry)

        return carry

    lax.fori_loop(0, Z, near_step, 0)
    gather_step(Z - 1, 0)

    @pl.when(z == 0)
    def _():
        hidden_step(Z - 1, 0)

    @pl.when(z == Z - 1)
    def _():
        hidden_step(0, 0)

    ring = pout.shape[0]
    big = Z * F
    near = jnp.minimum(jnp.where(z < Z - 1, z, big), jnp.where(z > 0, Z - 1 - z, big))
    count = Z * (F + Z - 1)

    def unit(n):
        s = n // Z
        i = lax.rem(n, Z)
        left_half = 2 * z < Z
        i = jnp.where(i == Z - 1, -1, i + jnp.where(i >= jnp.where(left_half, Z - 1 - z, z), 1, 0))
        d = jnp.where(i < 0, z, jnp.where(left_half, Z - 1 - i, i))
        away = jnp.where(d > z, z, jnp.where(d < z, Z - 1 - z, jnp.maximum(z, Z - 1 - z)))
        j = s - away
        return j, d, (j >= 0) & (j < F) & (n >= 0) & (n < count)

    def pair_copy(p, slot):
        return rdma(pout.at[p], pin.at[slot], pout_sem.at[p], pin_sem.at[slot], (f, partner))

    def sum_copy(p, slot, t):
        return rdma(sout.at[p], sin.at[slot], sout_sem.at[p], sin_sem.at[slot], (f, t))

    def produce(n, j, d, done):
        q = lax.rem(f + j, F)
        p = lax.rem(done, ring)
        he = hid_e[pl.ds(2 * d, 2)].reshape(2 * rows, H)
        hs = hid_s[pl.ds(2 * d, 2)].reshape(2 * rows, S)
        r = jnp.dot(he, wbuf[q, GU:GU + H, :], preferred_element_type=jnp.float32)
        r = r + jnp.dot(hs, wbuf[q, GU + H:ALL, :], preferred_element_type=jnp.float32)
        top, bottom = r[:rows], r[rows:]
        own[lax.rem(n, LAG + 1)] = jnp.where(c == 0, top, bottom)

        @pl.when(done >= ring)
        def _():
            pair_copy(p, 0).wait_send()

        pout[p] = jnp.where(c == 0, bottom, top).astype(jnp.bfloat16)
        pair_copy(p, j * Z + d).start()

    def finish(n, j, d, sent):
        q = lax.rem(f + j, F)
        o = lax.rem(n, LAG + 1)
        p = lax.rem(sent, ring)
        base = j * (Z + 1)
        pair_copy(0, j * Z + d).wait_recv()
        own[o] = own[o] + pin[j * Z + d].astype(jnp.float32)

        @pl.when((d >= z) & (z > 0))
        def _():
            sum_copy(0, base + d, me).wait_recv()
            own[o] = own[o] + sin[base + d].astype(jnp.float32)

        @pl.when((d <= z) & (z < Z - 1))
        def _():
            slot = base + jnp.where(d == z, Z, d)
            sum_copy(0, slot, me).wait_recv()
            own[o] = own[o] + sin[slot].astype(jnp.float32)

        @pl.when(d != z)
        def _():
            @pl.when(sent >= ring)
            def _():
                sum_copy(p, 0, partner).wait_send()

            sout[p] = own[o].astype(jnp.bfloat16)

            @pl.when(d > z)
            def _():
                sum_copy(p, base + d, right(me)).start()

            @pl.when(d < z)
            def _():
                sum_copy(p, base + jnp.where(d == z - 1, Z, d), left(me)).start()

        @pl.when(d == z)
        def _():
            mix[q] = own[o].astype(jnp.bfloat16)

    def sum_step(n, carry):
        done, sent = carry
        first = n // Z - near

        @pl.when((lax.rem(n, Z) == 0) & (first > 0) & (first < F))
        def _():
            w_copy(1, lax.rem(f + first, F), 1, f).wait_recv()

        j, d, valid = unit(n)

        @pl.when(valid)
        def _():
            produce(n, j, d, done)

        done = done + jnp.where(valid, 1, 0)
        m = n - LAG
        j, d, valid = unit(jnp.maximum(m, 0))
        valid = valid & (m >= 0)

        @pl.when(valid)
        def _():
            finish(m, j, d, sent)

        sent = sent + jnp.where(valid & (d != z), 1, 0)
        return done, sent

    lax.fori_loop(0, count + LAG, sum_step, (0, 0))

    for p in range(ring):
        pair_copy(p, 0).wait_send()
    for p in range(min(ring, (Z - 1) * F)):
        sum_copy(p, 0, partner).wait_send()
    for i in range(1, F):
        w_copy(0, f, i, lax.rem(f + i, F)).wait_send()
        w_copy(1, f, i, lax.rem(f + i, F)).wait_send()
    for i in range(1, T):
        wt_copy(me, i, lax.rem(me + i, T)).wait_send()

    def drain(k, carry):
        s = 2 * k + c

        @pl.when((k <= z) & (z < Z - 1))
        def _():
            tok_copy(s, 0, right(me)).wait_send()

        @pl.when((k >= z) & (z > 0))
        def _():
            tok_copy(s, 1, left(me)).wait_send()

        tok_copy(s, 2, partner).wait_send()
        return carry

    lax.fori_loop(0, Z, drain, 0)


def place(H, S, wbuf, mix, o_mixed, o_eg, o_eu, o_ed, o_sg, o_su, o_sd, sems):
    F, cw = wbuf.shape[0], wbuf.shape[2]
    GU = 2 * H + 2 * S
    pieces = ((o_eg, 0, H), (o_eu, H, H), (o_ed, GU, H), (o_sg, 2 * H, S), (o_su, 2 * H + S, S), (o_sd, GU + H, S))
    copies = []
    for p, (ref, lo, size) in enumerate(pieces):
        for q in range(F):
            copies.append(pltpu.make_async_copy(
                wbuf.at[q, lo:lo + size, :], ref.at[:, q * cw:(q + 1) * cw], sems.at[p, q]
            ))
    for q in range(F):
        copies.append(pltpu.make_async_copy(mix.at[q], o_mixed.at[:, q * cw:(q + 1) * cw], sems.at[6, q]))
    for copy in copies:
        copy.start()
    for copy in copies:
        copy.wait()


def local(F, T, tokens, gain, ex_gate, ex_up, ex_down, sh_gate, sh_up, sh_down, routes, route_weight):
    H, cw = ex_gate.shape[1:]
    S = sh_gate.shape[0]
    M = tokens.shape[0]
    D = tokens.shape[1]
    Z = T // 2
    N, U = (Z - 1) * F, Z * F
    ring = min(U, RING)
    bf, f32 = jnp.bfloat16, jnp.float32
    dma = pltpu.SemaphoreType.DMA
    wbuf, mix = pl.pallas_call(
        functools.partial(kernel, F, T, H, S, M),
        out_shape=[pltpu.VMEM((F, 3 * H + 3 * S, cw), bf), pltpu.VMEM((F, M, cw), bf)],
        in_specs=[pl.BlockSpec(memory_space=pltpu.VMEM)] * 2
        + [pl.BlockSpec(memory_space=pl.ANY)] * 6
        + [pl.BlockSpec(memory_space=pltpu.VMEM)] * 2,
        out_specs=[pl.BlockSpec(memory_space=pltpu.VMEM)] * 2,
        scratch_shapes=[
            pltpu.VMEM((T, M, D), bf),
            pltpu.VMEM((T, T, M), f32),
            pltpu.VMEM((T, M, H), bf),
            pltpu.VMEM((T, M, S), bf),
            pltpu.VMEM((LAG + 1, M, cw), f32),
            pltpu.VMEM((ring, M, cw), bf),
            pltpu.VMEM((U, M, cw), bf),
            pltpu.VMEM((ring, M, cw), bf),
            pltpu.VMEM((F * (Z + 1), M, cw), bf),
            dma((T, 3)),
            dma((T,)),
            dma((T,)),
            dma((T,)),
            dma((2, F)),
            dma((2, F)),
            dma((ring,)),
            dma((U,)),
            dma((ring,)),
            dma((F * (Z + 1),)),
            pltpu.VMEM((H, cw), f32),
            pltpu.VMEM((H, cw), f32),
            pltpu.VMEM((H, cw), f32),
            pltpu.VMEM((S, cw), f32),
            pltpu.VMEM((S, cw), f32),
            pltpu.VMEM((S, cw), f32),
            dma((6,)),
        ],
        compiler_params=pltpu.CompilerParams(
            collective_id=0, has_side_effects=True, vmem_limit_bytes=VMEM_LIMIT
        ),
    )(
        tokens, gain[None, :], ex_gate[0], ex_up[0], ex_down[0], sh_gate, sh_up, sh_down,
        routes.T, route_weight.T,
    )
    mixed, eg, eu, ed, sg, su, sd = pl.pallas_call(
        functools.partial(place, H, S),
        out_shape=[jax.ShapeDtypeStruct((M, D), bf)]
        + [jax.ShapeDtypeStruct((H, D), bf)] * 3
        + [jax.ShapeDtypeStruct((S, D), bf)] * 3,
        in_specs=[pl.BlockSpec(memory_space=pltpu.VMEM)] * 2,
        out_specs=[pl.BlockSpec(memory_space=pl.ANY)] * 7,
        scratch_shapes=[dma((7, F))],
        compiler_params=pltpu.CompilerParams(vmem_limit_bytes=4 << 20),
    )(pltpu.with_memory_space_constraint(wbuf, pltpu.VMEM), pltpu.with_memory_space_constraint(mix, pltpu.VMEM))
    return (mixed, eg[None], eu[None], ed[None], sg, su, sd)


def solution(mesh):
    in_specs = (
        P(("fs", "tp"), None),
        P("fs"),
        P("tp", None, "fs"),
        P("tp", None, "fs"),
        P("tp", None, "fs"),
        P("tp", "fs"),
        P("tp", "fs"),
        P("tp", "fs"),
        P(("fs", "tp"), None),
        P(("fs", "tp"), None),
    )
    out_specs = (
        P(("fs", "tp"), None),
        P("tp", None, None),
        P("tp", None, None),
        P("tp", None, None),
        P("tp", None),
        P("tp", None),
        P("tp", None),
    )
    step = functools.partial(local, mesh.shape["fs"], mesh.shape["tp"])
    return jax.shard_map(step, mesh=mesh, in_specs=in_specs, out_specs=out_specs, check_vma=False)
```
